32 devices in a mesh: ep: 8 (over z, x), tp: 4 (over y, core).
Axes of the slice: x: 2, y: 2, z: 4, core: 2. Of those that a mesh axis runs over, the one named last changes fastest.
Arguments:
- tokens: bfloat16 [384, 2048], P('ep'), may hold values from -6 to 6
- state: float32 [384, 8, 128, 128], P('ep', 'tp'), may hold values from -4 to 4
- norm_gain: float32 [2048], replicated, may hold values from 0.1 to 1.9
- w_query: bfloat16 [2048, 1024], P('ep', 'tp'), may hold values from -0.125 to 0.125
- w_forget: bfloat16 [2048, 1024], P('ep', 'tp'), may hold values from -0.125 to 0.125
- w_input: bfloat16 [2048, 1024], P('ep', 'tp'), may hold values from -0.125 to 0.125
- w_outgate: bfloat16 [2048, 1024], P('ep', 'tp'), may hold values from -0.125 to 0.125
- lower_bound: float32 [1024], P('tp'), may hold values from 0 to 0.9
- head_gain: float32 [1024], P('tp'), may hold values from 0.1 to 1.9
- w_output: bfloat16 [1024, 2048], P('tp'), may hold values from -0.1875 to 0.1875
- ffn_gain: float32 [2048], replicated, may hold values from 0.1 to 1.9
- route_ids: int32 [384, 4], P('ep'), may hold values from 0 to 15, all different within a row; in each aligned block of 48 rows (0 to 47, 48 to 95, ...) at most 24 rows name the same one
- route_weight: float32 [384, 4], P('ep'), may hold values from 0.2 to 1
- expert_gate: bfloat16 [16, 2048, 1024], P('ep', None, 'tp'), may hold values from -0.125 to 0.125
- expert_up: bfloat16 [16, 2048, 1024], P('ep', None, 'tp'), may hold values from -0.125 to 0.125
- expert_down: bfloat16 [16, 1024, 2048], P('ep', 'tp'), may hold values from -0.1875 to 0.1875
- shared_gate: bfloat16 [2048, 1024], P(None, 'tp'), may hold values from -0.125 to 0.125
- shared_up: bfloat16 [2048, 1024], P(None, 'tp'), may hold values from -0.125 to 0.125
- shared_down: bfloat16 [1024, 2048], P('tp'), may hold values from -0.1875 to 0.1875
- dense_gate: bfloat16 [2048, 8192], P('tp', 'ep'), may hold values from -0.125 to 0.125
- dense_up: bfloat16 [2048, 8192], P('tp', 'ep'), may hold values from -0.125 to 0.125
- dense_down: bfloat16 [8192, 2048], P('ep', 'tp'), may hold values from -0.0625 to 0.0625
- dense_mix: float32 [2048], P('tp'), may hold values from -6 to 6
Outputs:
- mixed: bfloat16 [384, 2048], P('ep', 'tp')
- new_state: float32 [384, 8, 128, 128], P('ep', 'tp')
The draws below stay inside these ranges and needn't reach their ends.
Inputs may be any that keep to these rules, and one draw needn't show every extreme that they name: `route_ids`: each row names 4 different experts. Among the rows of one device no expert is named more than 24 times, and in every draw some expert is named exactly 24 times by some device's rows.
All inputs are finite; a program needn't handle non-finite values.
Results may differ from the reference program's by a relative error of at most 0.025.
Values may be sent and summed in bfloat16 or wider, within the bound.
A program may use at most 64 MiB of HBM per device.

```python
import math
import jax
import jax.numpy as jnp
import numpy as np
from jax import lax

WIDTH = 2048
HEADS = 8
HEAD_DIM = 128
MIX_WIDTH = 1024
EXPERTS = 16
TOPK = 4
EXPERT_FF = 1024
SHARED_FF = 1024
DENSE_FF = 8192
SEQ_DEV = 48
BATCH = 384
CAP = 24
N_EP = 8
N_TP = 4


def shard_levels(rng, extent, cuts, smallest, largest):
    level = 1.0
    for axis_at, blocks in cuts:
        steps = jax.random.uniform(jax.random.fold_in(jax.random.fold_in(rng, 6), axis_at), (blocks,), jnp.float32, smallest / len(cuts), largest / len(cuts))
        level = level * jnp.repeat(jnp.exp(steps), extent[axis_at] // blocks).reshape((-1,) + (1,) * (len(extent) - 1 - axis_at))
    return level


def assign_block(key, own, number, rows, amount, top, limit, skew):
    order = jax.random.permutation(key, amount)
    crowded, usual = portions_of(amount, rows * top, limit, skew, True), portions_of(amount, rows * top, limit, skew, False)
    places = jnp.arange(amount)

    def named(tallies, turn):
        used = int((tallies > 0).sum())
        fixed = max(1, used // 4)
        moved = fixed + (places - fixed + turn * (used - fixed)) % max(1, amount - fixed)
        return jnp.zeros((amount,), jnp.int32).at[order[jnp.where(places < fixed, places, moved)]].set(jnp.asarray(tallies, jnp.int32))

    tallies = jnp.where(number % 4 == 0, named(crowded, number // 4), named(usual, number - number // 4 - 1))
    mixed = jax.random.permutation(jax.random.fold_in(own, 3), amount)
    giver, taker = mixed[0:amount // 2 * 2:2], mixed[1:amount // 2 * 2:2]
    room = jnp.minimum(tallies[giver] - 1, limit - tallies[taker]) // 2
    room = jnp.where((giver == order[0]) | (taker == order[0]) | (tallies[taker] == 0), 0, jnp.maximum(room, 0))
    moved = jax.random.randint(jax.random.fold_in(own, 4), (amount // 2,), 0, 1 << 20) % (room + 1)
    tallies = tallies.at[giver].add(-moved).at[taker].add(moved)
    members = jnp.searchsorted(jnp.cumsum(tallies), jnp.arange(rows * top), side="right").astype(jnp.int32)
    listing = members.reshape(top, rows).T
    listing = listing[jax.random.permutation(jax.random.fold_in(own, 1), rows)]
    turn = jax.random.randint(jax.random.fold_in(own, 2), (rows, 1), 0, top)
    return jnp.take_along_axis(listing, (jnp.arange(top)[None, :] + turn) % top, axis=1)


def portions_of(count, total, reach, skew, full):
    loads = [(1 << 20) // math.isqrt(rank ** skew) + 1 for rank in range(1, count + 1)]
    largest = reach if full else min(reach, max(-(-total // count), total * loads[0] // sum(loads)))
    least = 1 if total - largest >= count - 1 else 0
    holding, rest = [largest] + [least] * (count - 1), total - largest - least * (count - 1)
    while rest > 0:
        movable = [i for i in range(1, count) if holding[i] < largest] or [i for i in range(1, count) if holding[i] < reach]
        whole, remaining = sum([loads[i] for i in movable]), rest
        for i in movable:
            more = min(reach - holding[i], max(1, remaining * loads[i] // whole), rest)
            holding[i] = holding[i] + more
            rest = rest - more
    return np.array(holding)


def bell_draw(stream_key, shape, deviation, bound, cuts=(), held_as=jnp.bfloat16):
    result = deviation * jax.random.normal(stream_key, shape, jnp.float32)
    if cuts:
        result = result * shard_levels(stream_key, shape, cuts, -0.22, 0.18)
    return jnp.clip(result, -bound, bound).astype(held_as)


def setup_inputs(seed: int = 0) -> dict:
    keys = jax.random.split(jax.random.key(seed), 24)
    tokens = bell_draw(keys[0], (BATCH, WIDTH), 1.0, 6.0, ((0, 8),))
    state = bell_draw(keys[1], (BATCH, HEADS, HEAD_DIM, HEAD_DIM), 0.5, 4.0, ((0, 8), (1, 4)), jnp.float32)
    norm_gain = jnp.clip(1.0 + 0.18 * jax.random.normal(keys[2], (WIDTH,), jnp.float32), 0.1, 1.9)
    w_query = bell_draw(keys[3], (WIDTH, MIX_WIDTH), WIDTH ** -0.5, 0.125, ((0, 8), (1, 4)))
    w_forget = bell_draw(keys[4], (WIDTH, MIX_WIDTH), WIDTH ** -0.5, 0.125, ((0, 8), (1, 4)))
    w_input = bell_draw(keys[5], (WIDTH, MIX_WIDTH), WIDTH ** -0.5, 0.125, ((0, 8), (1, 4)))
    w_outgate = bell_draw(keys[6], (WIDTH, MIX_WIDTH), WIDTH ** -0.5, 0.125, ((0, 8), (1, 4)))
    lower_bound = jnp.clip(0.9 * jax.random.uniform(keys[7], (MIX_WIDTH,), jnp.float32) ** shard_levels(keys[7], (MIX_WIDTH,), ((0, 4),), -0.2, 0.2), 0.0, 0.9)
    head_gain = jnp.clip(1.0 + 0.18 * jax.random.normal(keys[8], (MIX_WIDTH,), jnp.float32), 0.1, 1.9)
    w_output = bell_draw(keys[9], (MIX_WIDTH, WIDTH), MIX_WIDTH ** -0.5, 0.1875, ((0, 4),))
    ffn_gain = jnp.clip(1.0 + 0.18 * jax.random.normal(keys[10], (WIDTH,), jnp.float32), 0.1, 1.9)
    route_ids_keys = jax.random.split(jax.random.fold_in(keys[11], 1), BATCH // SEQ_DEV)
    route_ids_turns = jax.random.permutation(jax.random.fold_in(keys[11], 3), BATCH // SEQ_DEV)
    route_ids = jax.vmap(lambda own, number: assign_block(jax.random.fold_in(keys[11], 2), own, number, SEQ_DEV, EXPERTS, TOPK, CAP, 2))(route_ids_keys, route_ids_turns).reshape((BATCH, TOPK))
    route_weight = jnp.clip(0.2 + 0.8 * jax.random.uniform(keys[12], (BATCH, TOPK), jnp.float32) ** shard_levels(keys[12], (BATCH, TOPK), ((0, 8),), -0.2, 0.2), 0.2, 1.0)
    expert_gate = bell_draw(keys[13], (EXPERTS, WIDTH, EXPERT_FF), WIDTH ** -0.5, 0.125, ((0, 8), (2, 4)))
    expert_up = bell_draw(keys[14], (EXPERTS, WIDTH, EXPERT_FF), WIDTH ** -0.5, 0.125, ((0, 8), (2, 4)))
    expert_down = bell_draw(keys[15], (EXPERTS, EXPERT_FF, WIDTH), EXPERT_FF ** -0.5, 0.1875, ((0, 8), (1, 4)))
    shared_gate = bell_draw(keys[16], (WIDTH, SHARED_FF), WIDTH ** -0.5, 0.125, ((1, 4),))
    shared_up = bell_draw(keys[17], (WIDTH, SHARED_FF), WIDTH ** -0.5, 0.125, ((1, 4),))
    shared_down = bell_draw(keys[18], (SHARED_FF, WIDTH), SHARED_FF ** -0.5, 0.1875, ((0, 4),))
    dense_gate = bell_draw(keys[19], (WIDTH, DENSE_FF), WIDTH ** -0.5, 0.125, ((0, 4), (1, 8)))
    dense_up = bell_draw(keys[20], (WIDTH, DENSE_FF), WIDTH ** -0.5, 0.125, ((0, 4), (1, 8)))
    dense_down = bell_draw(keys[21], (DENSE_FF, WIDTH), DENSE_FF ** -0.5, 0.0625, ((0, 8), (1, 4)))
    dense_mix = bell_draw(keys[22], (WIDTH,), 1.5, 6.0, ((0, 4),), jnp.float32)
    return dict(tokens=tokens, state=state, norm_gain=norm_gain, w_query=w_query, w_forget=w_forget, w_input=w_input, w_outgate=w_outgate, lower_bound=lower_bound, head_gain=head_gain, w_output=w_output, ffn_gain=ffn_gain, route_ids=route_ids, route_weight=route_weight, expert_gate=expert_gate, expert_up=expert_up, expert_down=expert_down, shared_gate=shared_gate, shared_up=shared_up, shared_down=shared_down, dense_gate=dense_gate, dense_up=dense_up, dense_down=dense_down, dense_mix=dense_mix)


EPS = 1e-06

def rms_scale(values, gain):
    values = values.astype(jnp.float32)
    return values * lax.rsqrt(lax.optimization_barrier(jnp.mean(values * values, axis=-1, keepdims=True)) + EPS) * gain

def rounded(values):
    return lax.optimization_barrier(values.astype(jnp.bfloat16)).astype(jnp.float32)

def blocked_sum(left, right, pieces):
    inner = left.shape[1] // pieces
    total = jnp.zeros((left.shape[0], right.shape[1]), jnp.float32)
    for index in range(pieces):
        part = jnp.dot(left[:, index * inner:(index + 1) * inner], right[index * inner:(index + 1) * inner], preferred_element_type=jnp.float32)
        total = total + rounded(part)
    return total

def reference(tokens, state, norm_gain, w_query, w_forget, w_input, w_outgate, lower_bound, head_gain, w_output, ffn_gain, route_ids, route_weight, expert_gate, expert_up, expert_down, shared_gate, shared_up, shared_down, dense_gate, dense_up, dense_down, dense_mix):
    batch = tokens.shape[0]
    normed = rms_scale(tokens, norm_gain).astype(jnp.bfloat16)

    def project(weight):
        return rounded(jnp.dot(normed, weight, preferred_element_type=jnp.float32))
    query, forget_pre, values, out_gate = [project(w) for w in (w_query, w_forget, w_input, w_outgate)]
    forget_sig = jax.nn.sigmoid(forget_pre)
    shape = (batch, HEADS, HEAD_DIM)
    decay = (lower_bound + (1.0 - lower_bound) * forget_sig).reshape(shape)
    keygate = ((1.0 - lower_bound) * (1.0 - forget_sig)).reshape(shape)
    new_state = decay[..., None] * state + keygate[..., None] * values.reshape(shape)[:, :, None, :]
    readout = jnp.einsum('bhk,bhkv->bhv', query.reshape(shape), new_state, precision=lax.Precision.HIGHEST)
    readout = readout * lax.rsqrt(lax.optimization_barrier(jnp.mean(readout * readout, axis=-1, keepdims=True)) + EPS)
    head_out = (readout.reshape(batch, MIX_WIDTH) * head_gain * jax.nn.silu(out_gate)).astype(jnp.bfloat16)
    resid = tokens.astype(jnp.float32) + blocked_sum(head_out, w_output, N_TP)
    moe_in = rms_scale(resid, ffn_gain).astype(jnp.bfloat16)
    flat_ids = route_ids.reshape(N_EP, SEQ_DEV * TOPK)
    onehot = (flat_ids[..., None] == jnp.arange(EXPERTS, dtype=jnp.int32)).astype(jnp.int32)
    slot_rank = lax.optimization_barrier(jnp.sum((jnp.cumsum(onehot, axis=1) - onehot) * onehot, axis=-1))
    device = jnp.arange(N_EP, dtype=jnp.int32)[:, None]
    slot_index = ((flat_ids * N_EP + device) * CAP + slot_rank).reshape(-1).astype(jnp.int32)
    token_index = jnp.repeat(jnp.arange(batch, dtype=jnp.int32), TOPK)
    table = jnp.full((EXPERTS * N_EP * CAP,), batch, jnp.int32).at[slot_index].set(token_index)
    padded = jnp.concatenate([moe_in, jnp.zeros((1, WIDTH), jnp.bfloat16)], axis=0)
    gathered = padded[table].reshape(EXPERTS, N_EP * CAP, WIDTH)

    def one_expert(args):
        rows_in, gate_weight, up_weight, down_weight = args
        gate_pre = jnp.dot(rows_in, gate_weight, preferred_element_type=jnp.float32)
        up_pre = jnp.dot(rows_in, up_weight, preferred_element_type=jnp.float32)
        hidden = (jax.nn.silu(gate_pre) * up_pre).astype(jnp.bfloat16)
        return blocked_sum(hidden, down_weight, N_TP).astype(jnp.bfloat16)
    outputs = lax.map(one_expert, (gathered, expert_gate, expert_up, expert_down)).reshape(-1, WIDTH)
    picked = outputs[slot_index].reshape(batch, TOPK, WIDTH).astype(jnp.float32)
    routed = lax.optimization_barrier(jnp.sum(route_weight[..., None] * picked, axis=1))
    shared_hidden = (jax.nn.silu(jnp.dot(moe_in, shared_gate, preferred_element_type=jnp.float32)) * jnp.dot(moe_in, shared_up, preferred_element_type=jnp.float32)).astype(jnp.bfloat16)
    shared_out = blocked_sum(shared_hidden, shared_down, N_TP)
    dense_pre_gate = blocked_sum(moe_in, dense_gate, N_TP)
    dense_pre_up = blocked_sum(moe_in, dense_up, N_TP)
    dense_hidden = (jax.nn.silu(dense_pre_gate) * dense_pre_up).astype(jnp.bfloat16)
    dense_out = jnp.dot(dense_hidden, dense_down, preferred_element_type=jnp.float32)
    mixed = (resid + routed + shared_out + jax.nn.sigmoid(dense_mix) * dense_out).astype(jnp.bfloat16)
    return (mixed, new_state)
```

```python
import functools

import jax
import jax.numpy as jnp
from jax import lax
from jax.experimental import pallas as pl
from jax.experimental.pallas import tpu as pltpu
from jax.sharding import PartitionSpec as P

EPS = 1e-06
LANES = 128
CORES = 2
F32 = jnp.float32
BF16 = jnp.bfloat16
VMEM_BYTES = 60 * 1024 * 1024


def send(src, dst, sems, slot, peer):
    send_sem, recv_sem = sems
    return pltpu.make_async_remote_copy(
        src_ref=src,
        dst_ref=dst,
        send_sem=send_sem.at[slot],
        recv_sem=recv_sem.at[slot],
        device_id=peer,
        device_id_type=pl.DeviceIdType.MESH,
    )


def span(index, size):
    return pl.ds(pl.multiple_of(index * size, size), size)


def greet(n, tpn, me, tp):
    barrier = pltpu.get_barrier_semaphore()
    for s in range(1, n):
        pl.semaphore_signal(
            barrier,
            inc=1,
            device_id={"ep": lax.rem(me + s, n)},
            device_id_type=pl.DeviceIdType.MESH,
        )
    for s in range(1, tpn):
        pl.semaphore_signal(
            barrier,
            inc=1,
            device_id={"tp": lax.rem(tp + s, tpn)},
            device_id_type=pl.DeviceIdType.MESH,
        )
    pl.semaphore_wait(barrier, n - 1 + tpn - 1)


def front_kernel(n, tpn, move, *refs):
    tokens, gain, route, mix, wq, wf, wi, wo = refs[:8]
    refs = refs[8:]
    if move:
        dgate, dup, ddown = refs[:3]
        refs = refs[3:]
    proj, route_all, mix_all = refs[:3]
    refs = refs[3:]
    if move:
        gate_out, up_out, down_out = refs[:3]
        refs = refs[3:]
    nsend, ncol, psend, precv = refs[:4]
    nsems, rsems, psems, msems = [(refs[4 + 2 * i], refs[5 + 2 * i]) for i in range(4)]
    refs = refs[12:]
    me = lax.axis_index("ep")
    tp = lax.axis_index("tp")
    seq = tokens.shape[0]
    depth = wq.shape[0]
    mixw = wq.shape[1]
    x = tokens[...].astype(F32)
    normed = (
        x * lax.rsqrt(jnp.mean(x * x, axis=-1, keepdims=True) + EPS) * gain[...]
    ).astype(BF16)
    for d in range(n):
        nsend[d] = normed[:, d * depth : (d + 1) * depth]
    greet(n, tpn, me, tp)
    ncopies, others = [None], []
    for s in range(1, n):
        peer = lax.rem(me + s, n)
        copy = send(nsend.at[peer], ncol.at[me], nsems, s, {"ep": peer})
        copy.start()
        ncopies.append(copy)
    if move:
        wsems = (refs[0], refs[1])
        lsems = refs[2]
        rows = dgate.shape[0]
        cols = gate_out.shape[1]
        drows = down_out.shape[0]
        dcols = ddown.shape[1]
        locals_ = []
        for s in range(tpn):
            peer = lax.rem(tp + s, tpn)
            for i, (a, b) in enumerate(
                (
                    (dgate.at[:, span(peer, cols)], gate_out.at[span(tp, rows), :]),
                    (dup.at[:, span(peer, cols)], up_out.at[span(tp, rows), :]),
                    (ddown.at[span(peer, drows), :], down_out.at[:, span(tp, dcols)]),
                )
            ):
                if s == 0:
                    copy = pltpu.make_async_copy(a, b, lsems.at[i])
                    locals_.append(copy)
                else:
                    copy = send(a, b, wsems, i * tpn + s, {"tp": peer})
                    others.append(copy)
                copy.start()
    for s in range(1, tpn):
        copy = send(mix, mix_all.at[tp], msems, s, {"tp": lax.rem(tp + s, tpn)})
        copy.start()
        others.append(copy)
    for s in range(1, n):
        copy = send(route, route_all.at[me], rsems, s, {"ep": lax.rem(me + s, n)})
        copy.start()
        others.append(copy)
    mix_all[tp] = mix[...]
    route_all[me] = route[...]

    def project(block):
        return [
            jnp.dot(block, w[...], preferred_element_type=F32).astype(BF16)
            for w in (wq, wf, wi, wo)
        ]

    pcopies = [None]
    for s in range(1, n):
        source = lax.rem(me + n - s, n)
        ncopies[s].wait_recv()
        for i, part in enumerate(project(ncol[source])):
            psend[source, :, i * mixw : (i + 1) * mixw] = part
        copy = send(psend.at[source], precv.at[me], psems, s, {"ep": source})
        copy.start()
        pcopies.append(copy)
    own = jnp.concatenate(project(nsend[me]), axis=1).astype(F32)
    for s in range(1, n):
        pcopies[s].wait_recv()
        own = own + precv[lax.rem(me + s, n)].astype(F32)
    proj[...] = own.astype(BF16)
    for s in range(1, n):
        ncopies[s].wait_send()
        pcopies[s].wait_send()
    for copy in others:
        copy.wait()
    if move:
        for copy in locals_:
            copy.wait()


def gather_kernel(
    n, tpn, tokens, gain, head, wout, resid, moe, hsend, hrecv, sqsend, sqrecv, *sems
):
    hsems, qsems, esems, ysems, csems = [(sems[2 * i], sems[2 * i + 1]) for i in range(5)]
    me = lax.axis_index("ep")
    tp = lax.axis_index("tp")
    seq, width = tokens.shape
    cols = width // tpn
    side, core = lax.div(tp, CORES), lax.rem(tp, CORES)
    sides = tpn // CORES
    twin = side * CORES + (CORES - 1 - core)
    for t in range(tpn):
        hsend[t] = jnp.dot(
            head[...], wout[:, t * cols : (t + 1) * cols], preferred_element_type=F32
        ).astype(BF16)
    greet(n, tpn, me, tp)
    hcopies = []
    for s in range(1, tpn):
        peer = lax.rem(tp + s, tpn)
        copy = send(hsend.at[peer], hrecv.at[tp], hsems, s, {"tp": peer})
        copy.start()
        hcopies.append(copy)
    total = hsend[tp].astype(F32)
    for s in range(1, tpn):
        hcopies[s - 1].wait_recv()
        total = total + hrecv[lax.rem(tp + tpn - s, tpn)].astype(F32)
    mine = span(tp, cols)
    total = tokens[:, mine].astype(F32) + total
    resid[...] = total
    square = jnp.broadcast_to(jnp.sum(total * total, axis=-1, keepdims=True), (seq, LANES))
    sqsend[...] = square
    qcopies = []
    for s in range(1, tpn):
        copy = send(sqsend, sqrecv.at[tp], qsems, s, {"tp": lax.rem(tp + s, tpn)})
        copy.start()
        qcopies.append(copy)
    for s in range(1, tpn):
        qcopies[s - 1].wait_recv()
        square = square + sqrecv[lax.rem(tp + tpn - s, tpn)]
    scale = lax.rsqrt(square[:, :1] / width + EPS)
    moe[span(me, seq), mine] = (total * scale * gain[:, mine]).astype(BF16)

    def block(e, t):
        return moe.at[span(e, seq), span(t, cols)]

    copies = []
    ecopies = [None]
    for s in range(1, n):
        copy = send(block(me, tp), block(me, tp), esems, s, {"ep": lax.rem(me + s, n)})
        copy.start()
        ecopies.append(copy)
    ycopies, ccopies = {}, {}
    for s in range(n):
        e = lax.rem(me + n - s, n)
        if s:
            ecopies[s].wait_recv()
        for q in range(1, sides):
            peer = lax.rem(side + q, sides) * CORES + core
            copy = send(block(e, tp), block(e, tp), ysems, s * sides + q, {"tp": peer})
            copy.start()
            ycopies[s, q] = copy
        copy = send(block(e, tp), block(e, tp), csems, s * sides, {"tp": twin})
        copy.start()
        ccopies[s, 0] = copy
    for s in range(n):
        e = lax.rem(me + n - s, n)
        for q in range(1, sides):
            ycopies[s, q].wait_recv()
            t = lax.rem(side + sides - q, sides) * CORES + core
            copy = send(block(e, t), block(e, t), csems, s * sides + q, {"tp": twin})
            copy.start()
            ccopies[s, q] = copy
    for copy in ccopies.values():
        copy.wait()
    for copy in list(ycopies.values()) + ecopies[1:] + hcopies + qcopies:
        copy.wait_send()


def reduce_kernel(
    n, tpn, part, shared, resid, out, crecv, ysend, yrecv, esend, erecv, *sems
):
    csems, ysems, esems = [(sems[2 * i], sems[2 * i + 1]) for i in range(3)]
    me = lax.axis_index("ep")
    tp = lax.axis_index("tp")
    seq, cols = resid.shape
    side, core = lax.div(tp, CORES), lax.rem(tp, CORES)
    sides = tpn // CORES
    twin = side * CORES + (CORES - 1 - core)
    greet(n, tpn, me, tp)
    order = list(range(1, n)) + [n, 0]

    def block(s, t):
        if s == n:
            return shared.at[:, span(t, cols)]
        return part.at[span(lax.rem(me + s, n), seq), span(t, cols)]

    turns = list(range(1, sides)) + [0]
    ccopies, ycopies, ecopies = {}, {}, {}
    for s in order:
        for q in turns:
            t = lax.rem(side + q, sides) * CORES + (CORES - 1 - core)
            i = s * sides + q
            copy = send(block(s, t), crecv.at[i], csems, i, {"tp": twin})
            copy.start()
            ccopies[s, q] = copy
    kept = {}
    for s in order:
        for q in turns[:-1]:
            peer = lax.rem(side + q, sides) * CORES + core
            i = s * sides + q
            ccopies[s, q].wait_recv()
            both = block(s, peer)[...].astype(F32) + crecv[i].astype(F32)
            ysend[i] = both.astype(BF16)
            copy = send(ysend.at[i], yrecv.at[i], ysems, i, {"tp": peer})
            copy.start()
            ycopies[s, q] = copy
    last = None
    for s in order:
        i = s * sides
        ccopies[s, 0].wait_recv()
        both = block(s, tp)[...].astype(F32) + crecv[i].astype(F32)
        for q in turns[:-1]:
            ycopies[s, q].wait_recv()
            both = both + yrecv[i + q].astype(F32)
        if 0 < s < n:
            esend[s] = both.astype(BF16)
            copy = send(esend.at[s], erecv.at[s], esems, s, {"ep": lax.rem(me + s, n)})
            copy.start()
            ecopies[s] = copy
        else:
            last = both if last is None else last + both
    last = last + resid[...]
    for s in range(1, n):
        ecopies[s].wait_recv()
        last = last + erecv[s].astype(F32)
    out[...] = last.astype(BF16)
    for group in (ccopies, ycopies, ecopies):
        for copy in group.values():
            copy.wait_send()


def pairs(counts):
    return [pltpu.SemaphoreType.DMA((c,)) for c in counts for _ in range(2)]


def call(kernel, outs, ins, spaces, out_spaces, scratch, ident):
    return pl.pallas_call(
        kernel,
        out_shape=outs,
        in_specs=[pl.BlockSpec(memory_space=s) for s in spaces],
        out_specs=[pl.BlockSpec(memory_space=s) for s in out_spaces],
        scratch_shapes=scratch,
        compiler_params=pltpu.CompilerParams(
            collective_id=ident, has_side_effects=True, vmem_limit_bytes=VMEM_BYTES
        ),
    )(*ins)


def local(
    tokens,
    state,
    norm_gain,
    w_query,
    w_forget,
    w_input,
    w_outgate,
    lower_bound,
    head_gain,
    w_output,
    ffn_gain,
    route_ids,
    route_weight,
    expert_gate,
    expert_up,
    expert_down,
    shared_gate,
    shared_up,
    shared_down,
    dense_gate,
    dense_up,
    dense_down,
    dense_mix,
):
    n = lax.axis_size("ep")
    tpn = lax.axis_size("tp")
    seq, width = tokens.shape
    depth, mix_local = w_query.shape
    heads_local = state.shape[1]
    head_dim = state.shape[2]
    cols = width // tpn
    exp_local = expert_gate.shape[0]
    experts = exp_local * n
    slots = -(-experts // LANES) * LANES
    sds = jax.ShapeDtypeStruct
    VM, ANY = pltpu.VMEM, pl.ANY

    route = jnp.sum(
        jnp.where(
            route_ids[:, :, None] == jnp.arange(slots, dtype=jnp.int32)[None, None, :],
            route_weight[:, :, None],
            jnp.float32(0.0),
        ),
        axis=1,
    )
    mix = jnp.broadcast_to(jax.nn.sigmoid(dense_mix)[None, :], (8, cols))
    dense_cols = dense_gate.shape[1] // tpn
    move = dense_cols % LANES == 0
    ins = [tokens, norm_gain[None, :], route, mix, w_query, w_forget, w_input, w_outgate]
    outs = [
        sds((seq, 4 * mix_local), BF16),
        sds((n, seq, slots), F32),
        sds((tpn, 8, cols), F32),
    ]
    scratch = [
        VM((n, seq, depth), BF16),
        VM((n, seq, depth), BF16),
        VM((n, seq, 4 * mix_local), BF16),
        VM((n, seq, 4 * mix_local), BF16),
    ] + pairs([n, n, n, tpn])
    spaces, out_spaces = [VM] * len(ins), [VM] * len(outs)
    if move:
        ins += [dense_gate, dense_up, dense_down]
        outs += [sds((width, dense_cols), BF16)] * 2 + [sds((dense_cols, width), BF16)]
        spaces += [ANY] * 3
        out_spaces += [ANY] * 3
        scratch += pairs([3 * tpn]) + [pltpu.SemaphoreType.DMA((3,))]
    res = call(
        functools.partial(front_kernel, n, tpn, move), outs, ins, spaces, out_spaces, scratch, 0
    )
    projected, route_all, mix_all = res[:3]
    if move:
        gate_w, up_w, down_w = res[3:]
    else:
        gate_w, up_w = [
            lax.all_to_all(w, "tp", split_axis=1, concat_axis=0, tiled=True)
            for w in (dense_gate, dense_up)
        ]
        down_w = lax.all_to_all(dense_down, "tp", split_axis=0, concat_axis=1, tiled=True)

    query, forget_pre, values, out_gate = jnp.split(projected.astype(F32), 4, axis=1)
    shape = (seq, heads_local, head_dim)
    forget_sig = jax.nn.sigmoid(forget_pre)
    decay = (lower_bound + (1.0 - lower_bound) * forget_sig).reshape(shape)
    keygate = ((1.0 - lower_bound) * (1.0 - forget_sig)).reshape(shape)
    new_state = decay[..., None] * state + keygate[..., None] * values.reshape(shape)[:, :, None, :]
    readout = jnp.einsum(
        "bhk,bhkv->bhv", query.reshape(shape), new_state, precision=lax.Precision.HIGHEST
    )
    readout = readout * lax.rsqrt(jnp.mean(readout * readout, axis=-1, keepdims=True) + EPS)
    head_out = (readout.reshape(seq, mix_local) * head_gain * jax.nn.silu(out_gate)).astype(BF16)

    sides = tpn // CORES
    resid, moe_in = call(
        functools.partial(gather_kernel, n, tpn),
        [sds((seq, cols), F32), sds((n * seq, width), BF16)],
        [tokens, ffn_gain[None, :], head_out, w_output],
        [VM] * 4,
        [VM] * 2,
        [
            VM((tpn, seq, cols), BF16),
            VM((tpn, seq, cols), BF16),
            VM((seq, LANES), F32),
            VM((tpn, seq, LANES), F32),
        ]
        + pairs([tpn, tpn, n, n * sides, n * sides]),
        1,
    )

    ep_index = lax.axis_index("ep")
    own = lax.dynamic_slice_in_dim(moe_in, ep_index * seq, seq, 0)
    shared_hidden = (
        jax.nn.silu(jnp.dot(own, shared_gate, preferred_element_type=F32))
        * jnp.dot(own, shared_up, preferred_element_type=F32)
    ).astype(BF16)
    shared_part = jnp.dot(shared_hidden, shared_down, preferred_element_type=F32).astype(BF16)

    route_rows = lax.dynamic_slice_in_dim(
        route_all.reshape(n * seq, slots), ep_index * exp_local, exp_local, 1
    )
    part = jnp.zeros((n * seq, width), F32)
    for e in range(exp_local):
        gate_pre = jnp.dot(moe_in, expert_gate[e], preferred_element_type=F32)
        up_pre = jnp.dot(moe_in, expert_up[e], preferred_element_type=F32)
        hidden = (jax.nn.silu(gate_pre) * up_pre * route_rows[:, e : e + 1]).astype(BF16)
        part = part + jnp.dot(hidden, expert_down[e], preferred_element_type=F32)
    dense_hidden = (
        jax.nn.silu(jnp.dot(moe_in, gate_w, preferred_element_type=F32))
        * jnp.dot(moe_in, up_w, preferred_element_type=F32)
    ).astype(BF16)
    mix_row = mix_all[:, 0, :].reshape(1, width)
    part = part + mix_row * jnp.dot(dense_hidden, down_w, preferred_element_type=F32)
    blocks = (n + 1) * sides
    (mixed,) = call(
        functools.partial(reduce_kernel, n, tpn),
        [sds((seq, cols), BF16)],
        [part.astype(BF16), shared_part, resid],
        [VM] * 3,
        [VM],
        [VM((blocks, seq, cols), BF16)] * 3 + [VM((n, seq, cols), BF16)] * 2
        + pairs([blocks, blocks, n]),
        2,
    )
    return (mixed, new_state)


def solution(mesh):
    placed = (
        P("ep", None),
        P("ep", "tp", None, None),
        P(),
        P("ep", "tp"),
        P("ep", "tp"),
        P("ep", "tp"),
        P("ep", "tp"),
        P("tp"),
        P("tp"),
        P("tp", None),
        P(),
        P("ep", None),
        P("ep", None),
        P("ep", None, "tp"),
        P("ep", None, "tp"),
        P("ep", "tp", None),
        P(None, "tp"),
        P(None, "tp"),
        P("tp", None),
        P("tp", "ep"),
        P("tp", "ep"),
        P("ep", "tp"),
        P("tp"),
    )
    return jax.shard_map(
        local,
        mesh=mesh,
        in_specs=placed,
        out_specs=(P("ep", "tp"), P("ep", "tp", None, None)),
        check_vma=False,
    )
```

```python
import functools

import jax
import jax.numpy as jnp
from jax import lax
from jax.experimental import pallas as pl
from jax.experimental.pallas import tpu as pltpu
from jax.sharding import PartitionSpec as P

EPS = 1e-06
LANES = 128
CORES = 2
F32 = jnp.float32
BF16 = jnp.bfloat16
VMEM_BYTES = 60 * 1024 * 1024


def send(src, dst, sems, slot, peer):
    send_sem, recv_sem = sems
    return pltpu.make_async_remote_copy(
        src_ref=src,
        dst_ref=dst,
        send_sem=send_sem.at[slot],
        recv_sem=recv_sem.at[slot],
        device_id=peer,
        device_id_type=pl.DeviceIdType.MESH,
    )


def span(index, size):
    return pl.ds(pl.multiple_of(index * size, size), size)


def greet(n, tpn, me, tp):
    barrier = pltpu.get_barrier_semaphore()
    for s in range(1, n):
        pl.semaphore_signal(
            barrier,
            inc=1,
            device_id={"ep": lax.rem(me + s, n)},
            device_id_type=pl.DeviceIdType.MESH,
        )
    for s in range(1, tpn):
        pl.semaphore_signal(
            barrier,
            inc=1,
            device_id={"tp": lax.rem(tp + s, tpn)},
            device_id_type=pl.DeviceIdType.MESH,
        )
    pl.semaphore_wait(barrier, n - 1 + tpn - 1)


def front_kernel(n, tpn, move, *refs):
    tokens, gain, route, mix, wq, wf, wi, wo = refs[:8]
    refs = refs[8:]
    if move:
        dgate, dup = refs[:2]
        refs = refs[2:]
    proj, route_all, mix_all = refs[:3]
    refs = refs[3:]
    if move:
        gate_out, up_out = refs[:2]
        refs = refs[2:]
    nsend, ncol, psend, precv = refs[:4]
    nsems, rsems, psems, msems = [(refs[4 + 2 * i], refs[5 + 2 * i]) for i in range(4)]
    refs = refs[12:]
    me = lax.axis_index("ep")
    tp = lax.axis_index("tp")
    seq = tokens.shape[0]
    depth = wq.shape[0]
    mixw = wq.shape[1]
    x = tokens[...].astype(F32)
    normed = (
        x * lax.rsqrt(jnp.mean(x * x, axis=-1, keepdims=True) + EPS) * gain[...]
    ).astype(BF16)
    for d in range(n):
        nsend[d] = normed[:, d * depth : (d + 1) * depth]
    greet(n, tpn, me, tp)
    ncopies, others = [None], []
    for s in range(1, n):
        peer = lax.rem(me + s, n)
        copy = send(nsend.at[peer], ncol.at[me], nsems, s, {"ep": peer})
        copy.start()
        ncopies.append(copy)
    if move:
        wsems = (refs[0], refs[1])
        lsems = refs[2]
        rows = dgate.shape[0]
        cols = gate_out.shape[1]
        locals_ = []
        for s in range(tpn):
            peer = lax.rem(tp + s, tpn)
            for i, (a, b) in enumerate(
                (
                    (dgate.at[:, span(peer, cols)], gate_out.at[span(tp, rows), :]),
                    (dup.at[:, span(peer, cols)], up_out.at[span(tp, rows), :]),
                )
            ):
                if s == 0:
                    copy = pltpu.make_async_copy(a, b, lsems.at[i])
                    locals_.append(copy)
                else:
                    copy = send(a, b, wsems, i * tpn + s, {"tp": peer})
                    others.append(copy)
                copy.start()
    for s in range(1, tpn):
        copy = send(mix, mix_all.at[tp], msems, s, {"tp": lax.rem(tp + s, tpn)})
        copy.start()
        others.append(copy)
    for s in range(1, n):
        copy = send(route, route_all.at[me], rsems, s, {"ep": lax.rem(me + s, n)})
        copy.start()
        others.append(copy)
    mix_all[tp] = mix[...]
    route_all[me] = route[...]

    def project(block):
        return [
            jnp.dot(block, w[...], preferred_element_type=F32).astype(BF16)
            for w in (wq, wf, wi, wo)
        ]

    pcopies = [None]
    for s in range(1, n):
        source = lax.rem(me + n - s, n)
        ncopies[s].wait_recv()
        for i, part in enumerate(project(ncol[source])):
            psend[source, :, i * mixw : (i + 1) * mixw] = part
        copy = send(psend.at[source], precv.at[me], psems, s, {"ep": source})
        copy.start()
        pcopies.append(copy)
    own = jnp.concatenate(project(nsend[me]), axis=1).astype(F32)
    for s in range(1, n):
        pcopies[s].wait_recv()
        own = own + precv[lax.rem(me + s, n)].astype(F32)
    proj[...] = own.astype(BF16)
    for s in range(1, n):
        ncopies[s].wait_send()
        pcopies[s].wait_send()
    for copy in others:
        copy.wait()
    if move:
        for copy in locals_:
            copy.wait()


def state_kernel(proj, bound, gain, state, new, head):
    rows, heads, dim = state.shape[:3]
    mixw = heads * dim
    p = proj[...].astype(F32)
    query, forget_pre, values, out_gate = [p[:, i * mixw : (i + 1) * mixw] for i in range(4)]
    sig = jax.nn.sigmoid(forget_pre)
    low = bound[...]
    decay = low + (1.0 - low) * sig
    keygate = (1.0 - low) * (1.0 - sig)
    scale = gain[...] * (out_gate * jax.nn.sigmoid(out_gate))
    for h in range(heads):
        part = slice(h * dim, (h + 1) * dim)
        dt, kt, qt = [jnp.transpose(a[:, part]) for a in (decay, keygate, query)]
        reads = []
        for b in range(rows):
            fresh = dt[:, b : b + 1] * state[b, h] + kt[:, b : b + 1] * values[b : b + 1, part]
            new[b, h] = fresh
            reads.append(jnp.sum(qt[:, b : b + 1] * fresh, axis=0, keepdims=True))
        read = jnp.concatenate(reads, axis=0)
        read = read * lax.rsqrt(jnp.mean(read * read, axis=-1, keepdims=True) + EPS)
        head[:, part] = (read * scale[:, part]).astype(BF16)


def main_kernel(n, tpn, move, *refs):
    tokens, gain, head, wout, route, mix = refs[:6]
    hbm = refs[6:15]
    out = refs[15]
    moe, resid, hsend, hrecv, sqsend, sqrecv = refs[16:22]
    held = refs[22:31]
    part, spart, crecv, ysend, yrecv, esend, erecv = refs[31:38]
    sems = refs[38:]
    hsems, qsems, esems, ysems, csems, c2sems, y2sems, e2sems, wsems = [
        (sems[2 * i], sems[2 * i + 1]) for i in range(9)
    ]
    lsems = sems[18]
    egate, eup, edown, sgate, sup, sdown, dgate, dup, ddown = held
    me = lax.axis_index("ep")
    tp = lax.axis_index("tp")
    seq, width = tokens.shape
    cols = width // tpn
    side, core = lax.div(tp, CORES), lax.rem(tp, CORES)
    sides = tpn // CORES
    twin = side * CORES + (CORES - 1 - core)
    exp_local = egate.shape[0]
    for t in range(tpn):
        hsend[t] = jnp.dot(
            head[...], wout[:, t * cols : (t + 1) * cols], preferred_element_type=F32
        ).astype(BF16)
    greet(n, tpn, me, tp)
    hcopies = []
    for s in range(1, tpn):
        peer = lax.rem(tp + s, tpn)
        copy = send(hsend.at[peer], hrecv.at[tp], hsems, s, {"tp": peer})
        copy.start()
        hcopies.append(copy)
    fetches = []
    drows = ddown.shape[0]
    for i in range(9):
        src, dst = hbm[i], held[i]
        if move and i == 8:
            src, dst = src.at[span(tp, drows), :], dst.at[:, span(tp, cols)]
        copy = pltpu.make_async_copy(src, dst, lsems.at[i])
        copy.start()
        fetches.append(copy)
    total = hsend[tp].astype(F32)
    for s in range(1, tpn):
        hcopies[s - 1].wait_recv()
        total = total + hrecv[lax.rem(tp + tpn - s, tpn)].astype(F32)
    mine = span(tp, cols)
    total = tokens[:, mine].astype(F32) + total
    resid[...] = total
    square = jnp.broadcast_to(jnp.sum(total * total, axis=-1, keepdims=True), (seq, LANES))
    sqsend[...] = square
    qcopies = []
    for s in range(1, tpn):
        copy = send(sqsend, sqrecv.at[tp], qsems, s, {"tp": lax.rem(tp + s, tpn)})
        copy.start()
        qcopies.append(copy)
    for s in range(1, tpn):
        qcopies[s - 1].wait_recv()
        square = square + sqrecv[lax.rem(tp + tpn - s, tpn)]
    scale = lax.rsqrt(square[:, :1] / width + EPS)
    moe[span(me, seq), mine] = (total * scale * gain[:, mine]).astype(BF16)

    def block(e, t):
        return moe.at[span(e, seq), span(t, cols)]

    ecopies = [None]
    for s in range(1, n):
        copy = send(block(me, tp), block(me, tp), esems, s, {"ep": lax.rem(me + s, n)})
        copy.start()
        ecopies.append(copy)
    ycopies, ccopies = {}, {}
    for s in range(n):
        e = lax.rem(me + n - s, n)
        if s:
            ecopies[s].wait_recv()
        for q in range(1, sides):
            peer = lax.rem(side + q, sides) * CORES + core
            copy = send(block(e, tp), block(e, tp), ysems, s * sides + q, {"tp": peer})
            copy.start()
            ycopies[s, q] = copy
        copy = send(block(e, tp), block(e, tp), csems, s * sides, {"tp": twin})
        copy.start()
        ccopies[s, 0] = copy
    wcopies = []
    if move:
        for s in range(1, tpn):
            peer = lax.rem(tp + s, tpn)
            copy = send(
                hbm[8].at[span(peer, drows), :], ddown.at[:, span(tp, cols)], wsems, s, {"tp": peer}
            )
            copy.start()
            wcopies.append(copy)
    for s in range(n):
        e = lax.rem(me + n - s, n)
        for q in range(1, sides):
            ycopies[s, q].wait_recv()
            t = lax.rem(side + sides - q, sides) * CORES + core
            copy = send(block(e, t), block(e, t), csems, s * sides + q, {"tp": twin})
            copy.start()
            ccopies[s, q] = copy
    for copy in ccopies.values():
        copy.wait()
    for copy in fetches:
        copy.wait()

    def swiglu(rows, gate, up):
        gate_pre = jnp.dot(rows, gate, preferred_element_type=F32)
        return gate_pre * jax.nn.sigmoid(gate_pre) * jnp.dot(rows, up, preferred_element_type=F32)

    rows = moe[...]
    lane = lax.broadcasted_iota(jnp.int32, (n * seq, route.shape[-1]), 1)
    weights = route[...].reshape(n * seq, route.shape[-1])
    hidden = []
    for e in range(exp_local):
        weight = jnp.sum(
            jnp.where(lane == me * exp_local + e, weights, 0.0), axis=1, keepdims=True
        )
        hidden.append((swiglu(rows, egate[e], eup[e]) * weight).astype(BF16))
    dense = swiglu(rows, dgate[...], dup[...]).astype(BF16)
    shared = swiglu(moe[span(me, seq), :], sgate[...], sup[...]).astype(BF16)
    for copy in wcopies:
        copy.wait()

    def compute(t):
        at = span(t, cols)
        value = mix[t, 0:1, :] * jnp.dot(dense, ddown[:, at], preferred_element_type=F32)
        for e in range(exp_local):
            value = value + jnp.dot(hidden[e], edown[e, :, at], preferred_element_type=F32)
        part[t] = value.astype(BF16)
        spart[t] = jnp.dot(shared, sdown[:, at], preferred_element_type=F32).astype(BF16)

    order = list(range(1, n)) + [n, 0]
    turns = list(range(1, sides)) + [0]

    def piece(s, t):
        if s == n:
            return spart.at[t]
        return part.at[t, span(lax.rem(me + s, n), seq), :]

    c2, y2, e2 = {}, {}, {}
    last = None
    for q in turns:
        other = lax.rem(side + q, sides) * CORES + (CORES - 1 - core)
        compute(other)
        for s in order:
            i = s * sides + q
            copy = send(piece(s, other), crecv.at[i], c2sems, i, {"tp": twin})
            copy.start()
            c2[s, q] = copy
        peer = lax.rem(side + q, sides) * CORES + core
        compute(peer)
        for s in order:
            i = s * sides + q
            c2[s, q].wait_recv()
            both = piece(s, peer)[...].astype(F32) + crecv[i].astype(F32)
            if q:
                ysend[i] = both.astype(BF16)
                copy = send(ysend.at[i], yrecv.at[i], y2sems, i, {"tp": peer})
                copy.start()
                y2[s, q] = copy
                continue
            for z in turns[:-1]:
                y2[s, z].wait_recv()
                both = both + yrecv[i + z].astype(F32)
            if 0 < s < n:
                esend[s] = both.astype(BF16)
                copy = send(esend.at[s], erecv.at[s], e2sems, s, {"ep": lax.rem(me + s, n)})
                copy.start()
                e2[s] = copy
            else:
                last = both if last is None else last + both
    last = last + resid[...]
    for s in range(1, n):
        e2[s].wait_recv()
        last = last + erecv[s].astype(F32)
    out[...] = last.astype(BF16)
    for copy in list(ycopies.values()) + ecopies[1:] + hcopies + qcopies:
        copy.wait_send()
    for group in (c2, y2, e2):
        for copy in group.values():
            copy.wait_send()


def pairs(counts):
    return [pltpu.SemaphoreType.DMA((c,)) for c in counts for _ in range(2)]


def call(kernel, outs, ins, spaces, out_spaces, scratch, ident):
    return pl.pallas_call(
        kernel,
        out_shape=outs,
        in_specs=[pl.BlockSpec(memory_space=s) for s in spaces],
        out_specs=[pl.BlockSpec(memory_space=s) for s in out_spaces],
        scratch_shapes=scratch,
        compiler_params=pltpu.CompilerParams(
            collective_id=ident, has_side_effects=True, vmem_limit_bytes=VMEM_BYTES
        ),
    )(*ins)


def local(
    tokens,
    state,
    norm_gain,
    w_query,
    w_forget,
    w_input,
    w_outgate,
    lower_bound,
    head_gain,
    w_output,
    ffn_gain,
    route_ids,
    route_weight,
    expert_gate,
    expert_up,
    expert_down,
    shared_gate,
    shared_up,
    shared_down,
    dense_gate,
    dense_up,
    dense_down,
    dense_mix,
):
    n = lax.axis_size("ep")
    tpn = lax.axis_size("tp")
    seq, width = tokens.shape
    depth, mix_local = w_query.shape
    heads_local = state.shape[1]
    head_dim = state.shape[2]
    cols = width // tpn
    exp_local = expert_gate.shape[0]
    experts = exp_local * n
    slots = -(-experts // LANES) * LANES
    sds = jax.ShapeDtypeStruct
    VM, ANY = pltpu.VMEM, pl.ANY

    route = jnp.sum(
        jnp.where(
            route_ids[:, :, None] == jnp.arange(slots, dtype=jnp.int32)[None, None, :],
            route_weight[:, :, None],
            jnp.float32(0.0),
        ),
        axis=1,
    )
    mix = jnp.broadcast_to(jax.nn.sigmoid(dense_mix)[None, :], (8, cols))
    dense_cols = dense_gate.shape[1] // tpn
    move = dense_cols % LANES == 0
    ins = [tokens, norm_gain[None, :], route, mix, w_query, w_forget, w_input, w_outgate]
    outs = [
        sds((seq, 4 * mix_local), BF16),
        sds((n, seq, slots), F32),
        sds((tpn, 8, cols), F32),
    ]
    scratch = [
        VM((n, seq, depth), BF16),
        VM((n, seq, depth), BF16),
        VM((n, seq, 4 * mix_local), BF16),
        VM((n, seq, 4 * mix_local), BF16),
    ] + pairs([n, n, n, tpn])
    spaces, out_spaces = [VM] * len(ins), [VM] * len(outs)
    if move:
        ins += [dense_gate, dense_up]
        outs += [sds((width, dense_cols), BF16)] * 2
        spaces += [ANY] * 2
        out_spaces += [ANY] * 2
        scratch += pairs([2 * tpn]) + [pltpu.SemaphoreType.DMA((2,))]
    res = call(
        functools.partial(front_kernel, n, tpn, move), outs, ins, spaces, out_spaces, scratch, 0
    )
    projected, route_all, mix_all = res[:3]
    if move:
        gate_w, up_w = res[3:]
        down_w = dense_down
    else:
        gate_w, up_w = [
            lax.all_to_all(w, "tp", split_axis=1, concat_axis=0, tiled=True)
            for w in (dense_gate, dense_up)
        ]
        down_w = lax.all_to_all(dense_down, "tp", split_axis=0, concat_axis=1, tiled=True)

    step = 8
    new_state, head_out = pl.pallas_call(
        state_kernel,
        grid=(seq // step,),
        out_shape=[sds(state.shape, F32), sds((seq, mix_local), BF16)],
        in_specs=[
            pl.BlockSpec((step, 4 * mix_local), lambda i: (i, 0)),
            pl.BlockSpec((1, mix_local), lambda i: (0, 0)),
            pl.BlockSpec((1, mix_local), lambda i: (0, 0)),
            pl.BlockSpec((step,) + state.shape[1:], lambda i: (i, 0, 0, 0)),
        ],
        out_specs=[
            pl.BlockSpec((step,) + state.shape[1:], lambda i: (i, 0, 0, 0)),
            pl.BlockSpec((step, mix_local), lambda i: (i, 0)),
        ],
    )(projected, lower_bound[None, :], head_gain[None, :], state)

    sides = tpn // CORES
    blocks = (n + 1) * sides
    big = [expert_gate, expert_up, expert_down, shared_gate, shared_up, shared_down]
    big += [gate_w, up_w, down_w]
    held = [VM(w.shape, BF16) for w in big]
    if move:
        held[8] = VM((dense_cols, width), BF16)
    (mixed,) = call(
        functools.partial(main_kernel, n, tpn, move),
        [sds((seq, cols), BF16)],
        [tokens, ffn_gain[None, :], head_out, w_output, route_all, mix_all] + big,
        [VM] * 6 + [ANY] * 9,
        [VM],
        [
            VM((n * seq, width), BF16),
            VM((seq, cols), F32),
            VM((tpn, seq, cols), BF16),
            VM((tpn, seq, cols), BF16),
            VM((seq, LANES), F32),
            VM((tpn, seq, LANES), F32),
        ]
        + held
        + [VM((tpn, n * seq, cols), BF16), VM((tpn, seq, cols), BF16)]
        + [VM((blocks, seq, cols), BF16)] * 3
        + [VM((n, seq, cols), BF16)] * 2
        + pairs([tpn, tpn, n, n * sides, n * sides, blocks, blocks, n, tpn])
        + [pltpu.SemaphoreType.DMA((9,))],
        1,
    )
    return (mixed, new_state)


def solution(mesh):
    placed = (
        P("ep", None),
        P("ep", "tp", None, None),
        P(),
        P("ep", "tp"),
        P("ep", "tp"),
        P("ep", "tp"),
        P("ep", "tp"),
        P("tp"),
        P("tp"),
        P("tp", None),
        P(),
        P("ep", None),
        P("ep", None),
        P("ep", None, "tp"),
        P("ep", None, "tp"),
        P("ep", "tp", None),
        P(None, "tp"),
        P(None, "tp"),
        P("tp", None),
        P("tp", "ep"),
        P("tp", "ep"),
        P("ep", "tp"),
        P("tp"),
    )
    return jax.shard_map(
        local,
        mesh=mesh,
        in_specs=placed,
        out_specs=(P("ep", "tp"), P("ep", "tp", None, None)),
        check_vma=False,
    )
```

```python
import functools

import jax
import jax.numpy as jnp
from jax import lax
from jax.experimental import pallas as pl
from jax.experimental.pallas import tpu as pltpu
from jax.sharding import PartitionSpec as P

EPS = 1e-06
LANES = 128
CORES = 2
F32 = jnp.float32
BF16 = jnp.bfloat16
VMEM_BYTES = 60 * 1024 * 1024


def send(src, dst, sems, slot, peer):
    send_sem, recv_sem = sems
    return pltpu.make_async_remote_copy(
        src_ref=src,
        dst_ref=dst,
        send_sem=send_sem.at[slot],
        recv_sem=recv_sem.at[slot],
        device_id=peer,
        device_id_type=pl.DeviceIdType.MESH,
    )


def span(index, size):
    return pl.ds(pl.multiple_of(index * size, size), size)


def ring(n, me):
    half = n // 2
    z, x = lax.div(me, 2), lax.rem(me, 2)

    def peer(s, f):
        return lax.rem(z + s, half) * 2 + lax.rem(x + f, 2)

    def source(s, f):
        return lax.rem(z + half - s, half) * 2 + lax.rem(x + f, 2)

    return half, peer, source, source(0, 1)


def greet(n, tpn, me, tp):
    barrier = pltpu.get_barrier_semaphore()
    for s in range(1, n):
        pl.semaphore_signal(
            barrier,
            inc=1,
            device_id={"ep": lax.rem(me + s, n)},
            device_id_type=pl.DeviceIdType.MESH,
        )
    for s in range(1, tpn):
        pl.semaphore_signal(
            barrier,
            inc=1,
            device_id={"tp": lax.rem(tp + s, tpn)},
            device_id_type=pl.DeviceIdType.MESH,
        )
    pl.semaphore_wait(barrier, n - 1 + tpn - 1)


def front_kernel(n, tpn, move, *refs):
    tokens, gain, ids, weight, premix, wq, wf, wi, wo = refs[:9]
    refs = refs[9:]
    if move:
        dgate, dup = refs[:2]
        refs = refs[2:]
    proj, route_all, mix_all = refs[:3]
    refs = refs[3:]
    if move:
        gate_out, up_out = refs[:2]
        refs = refs[2:]
    route, mix, nsend, ncol, psend, precv, xrecv = refs[:7]
    nsems, rsems, psems, msems, xsems = [(refs[7 + 2 * i], refs[8 + 2 * i]) for i in range(5)]
    refs = refs[17:]
    me = lax.axis_index("ep")
    tp = lax.axis_index("tp")
    seq = tokens.shape[0]
    depth = wq.shape[0]
    mixw = wq.shape[1]
    x = tokens[...].astype(F32)
    normed = (
        x * lax.rsqrt(jnp.mean(x * x, axis=-1, keepdims=True) + EPS) * gain[...]
    ).astype(BF16)
    for d in range(n):
        nsend[d] = normed[:, d * depth : (d + 1) * depth]
    lane = lax.broadcasted_iota(jnp.int32, route.shape, 1)
    table = jnp.zeros(route.shape, F32)
    for k in range(ids.shape[1]):
        table = table + jnp.where(lane == ids[:, k : k + 1], weight[:, k : k + 1], 0.0)
    route[...] = table
    mix[...] = jnp.broadcast_to(jax.nn.sigmoid(premix[...]), mix.shape)
    half, to, source, mate = ring(n, me)
    greet(n, tpn, me, tp)
    ncopies, others = {}, []
    for f in (1, 0):
        for s in list(range(1, half)) + [0]:
            if s or f:
                peer = to(s, f)
                copy = send(nsend.at[peer], ncol.at[me], nsems, 2 * s + f, {"ep": peer})
                copy.start()
                ncopies[s, f] = copy
    if move:
        wsems = (refs[0], refs[1])
        lsems = refs[2]
        rows = dgate.shape[0]
        cols = gate_out.shape[1]
        locals_ = []
        for s in range(tpn):
            peer = lax.rem(tp + s, tpn)
            for i, (a, b) in enumerate(
                (
                    (dgate.at[:, span(peer, cols)], gate_out.at[span(tp, rows), :]),
                    (dup.at[:, span(peer, cols)], up_out.at[span(tp, rows), :]),
                )
            ):
                if s == 0:
                    copy = pltpu.make_async_copy(a, b, lsems.at[i])
                    locals_.append(copy)
                else:
                    copy = send(a, b, wsems, i * tpn + s, {"tp": peer})
                    others.append(copy)
                copy.start()
    for s in range(1, tpn):
        copy = send(mix, mix_all.at[tp], msems, s, {"tp": lax.rem(tp + s, tpn)})
        copy.start()
        others.append(copy)
    for s in range(1, n):
        copy = send(route, route_all.at[me], rsems, s, {"ep": lax.rem(me + s, n)})
        copy.start()
        others.append(copy)
    mix_all[tp] = mix[...]
    route_all[me] = route[...]

    def project(block):
        return [
            jnp.dot(block, w[...], preferred_element_type=F32).astype(BF16)
            for w in (wq, wf, wi, wo)
        ]

    pcopies, xcopies = {}, {}
    turns = list(range(1, half)) + [0]
    for s in turns:
        d = source(s, 1)
        ncopies[s, 1].wait_recv()
        for i, part in enumerate(project(ncol[d])):
            psend[d, :, i * mixw : (i + 1) * mixw] = part
        copy = send(psend.at[d], xrecv.at[s], xsems, s, {"ep": mate})
        copy.start()
        xcopies[s] = copy
    for s in turns:
        d = source(s, 0)
        if s:
            ncopies[s, 0].wait_recv()
        own = jnp.concatenate(project(ncol[d] if s else nsend[me]), axis=1).astype(F32)
        xcopies[s].wait_recv()
        own = own + xrecv[s].astype(F32)
        if s:
            psend[d] = own.astype(BF16)
            copy = send(psend.at[d], precv.at[s], psems, s, {"ep": d})
            copy.start()
            pcopies[s] = copy
    for s in range(1, half):
        pcopies[s].wait_recv()
        own = own + precv[s].astype(F32)
    proj[...] = own.astype(BF16)
    for group in (ncopies, xcopies, pcopies):
        for copy in group.values():
            copy.wait_send()
    for copy in others:
        copy.wait()
    if move:
        for copy in locals_:
            copy.wait()


def state_kernel(proj, bound, gain, state, new, head):
    rows, heads, dim = state.shape[:3]
    mixw = heads * dim
    p = proj[...].astype(F32)
    query, forget_pre, values, out_gate = [p[:, i * mixw : (i + 1) * mixw] for i in range(4)]
    sig = jax.nn.sigmoid(forget_pre)
    low = bound[...]
    decay = low + (1.0 - low) * sig
    keygate = (1.0 - low) * (1.0 - sig)
    scale = gain[...] * (out_gate * jax.nn.sigmoid(out_gate))
    for h in range(heads):
        part = slice(h * dim, (h + 1) * dim)
        dt, kt, qt = [jnp.transpose(a[:, part]) for a in (decay, keygate, query)]
        reads = []
        for b in range(rows):
            fresh = dt[:, b : b + 1] * state[b, h] + kt[:, b : b + 1] * values[b : b + 1, part]
            new[b, h] = fresh
            reads.append(jnp.sum(qt[:, b : b + 1] * fresh, axis=0, keepdims=True))
        read = jnp.concatenate(reads, axis=0)
        read = read * lax.rsqrt(jnp.mean(read * read, axis=-1, keepdims=True) + EPS)
        head[:, part] = (read * scale[:, part]).astype(BF16)


def main_kernel(n, tpn, move, *refs):
    tokens, gain, head, wout, route, mix = refs[:6]
    hbm = refs[6:15]
    out = refs[15]
    moe, resid, hsend, hrecv, sqsend, sqrecv = refs[16:22]
    held = refs[22:31]
    part, spart, crecv, ysend, yrecv, esend, erecv, xrecv = refs[31:39]
    sems = refs[39:]
    hsems, qsems, esems, ysems, csems, c2sems, y2sems, e2sems, wsems, xsems, x2sems = [
        (sems[2 * i], sems[2 * i + 1]) for i in range(11)
    ]
    lsems = sems[22]
    egate, eup, edown, sgate, sup, sdown, dgate, dup, ddown = held
    me = lax.axis_index("ep")
    tp = lax.axis_index("tp")
    seq, width = tokens.shape
    cols = width // tpn
    side, core = lax.div(tp, CORES), lax.rem(tp, CORES)
    sides = tpn // CORES
    twin = side * CORES + (CORES - 1 - core)
    exp_local = egate.shape[0]
    for t in range(tpn):
        hsend[t] = jnp.dot(
            head[...], wout[:, t * cols : (t + 1) * cols], preferred_element_type=F32
        ).astype(BF16)
    greet(n, tpn, me, tp)
    hcopies = []
    for s in range(1, tpn):
        peer = lax.rem(tp + s, tpn)
        copy = send(hsend.at[peer], hrecv.at[tp], hsems, s, {"tp": peer})
        copy.start()
        hcopies.append(copy)
    fetches = []
    drows = ddown.shape[0]
    for i in range(9):
        src, dst = hbm[i], held[i]
        if move and i == 8:
            src, dst = src.at[span(tp, drows), :], dst.at[:, span(tp, cols)]
        copy = pltpu.make_async_copy(src, dst, lsems.at[i])
        copy.start()
        fetches.append(copy)
    total = hsend[tp].astype(F32)
    for s in range(1, tpn):
        hcopies[s - 1].wait_recv()
        total = total + hrecv[lax.rem(tp + tpn - s, tpn)].astype(F32)
    mine = span(tp, cols)
    total = tokens[:, mine].astype(F32) + total
    resid[...] = total
    square = jnp.broadcast_to(jnp.sum(total * total, axis=-1, keepdims=True), (seq, LANES))
    sqsend[...] = square
    qcopies = []
    for s in range(1, tpn):
        copy = send(sqsend, sqrecv.at[tp], qsems, s, {"tp": lax.rem(tp + s, tpn)})
        copy.start()
        qcopies.append(copy)
    for s in range(1, tpn):
        qcopies[s - 1].wait_recv()
        square = square + sqrecv[lax.rem(tp + tpn - s, tpn)]
    scale = lax.rsqrt(square[:, :1] / width + EPS)
    moe[span(me, seq), mine] = (total * scale * gain[:, mine]).astype(BF16)

    def block(e, t):
        return moe.at[span(e, seq), span(t, cols)]

    half, to, source, mate = ring(n, me)
    ecopies, xcopies, ycopies, ccopies = {}, {}, {}, {}
    for s in range(1, half):
        copy = send(block(me, tp), block(me, tp), esems, s, {"ep": to(s, 0)})
        copy.start()
        ecopies[s] = copy

    def spread(s, f):
        e, u = source(s, f), 2 * s + f
        for q in range(1, sides):
            peer = lax.rem(side + q, sides) * CORES + core
            copy = send(block(e, tp), block(e, tp), ysems, u * sides + q, {"tp": peer})
            copy.start()
            ycopies[u, q] = copy
        copy = send(block(e, tp), block(e, tp), csems, u * sides, {"tp": twin})
        copy.start()
        ccopies[u, 0] = copy

    for s in range(half):
        e = source(s, 0)
        if s:
            ecopies[s].wait_recv()
        copy = send(block(e, tp), block(e, tp), xsems, s, {"ep": mate})
        copy.start()
        xcopies[s] = copy
        spread(s, 0)
    for s in range(half):
        xcopies[s].wait_recv()
        spread(s, 1)
    wcopies = []
    if move:
        for s in range(1, tpn):
            peer = lax.rem(tp + s, tpn)
            copy = send(
                hbm[8].at[span(peer, drows), :], ddown.at[:, span(tp, cols)], wsems, s, {"tp": peer}
            )
            copy.start()
            wcopies.append(copy)
    for u in [2 * s for s in range(half)] + [2 * s + 1 for s in range(half)]:
        e = source(u // 2, u % 2)
        for q in range(1, sides):
            ycopies[u, q].wait_recv()
            t = lax.rem(side + sides - q, sides) * CORES + core
            copy = send(block(e, t), block(e, t), csems, u * sides + q, {"tp": twin})
            copy.start()
            ccopies[u, q] = copy
    for copy in ccopies.values():
        copy.wait()
    for copy in fetches:
        copy.wait()

    def swiglu(rows, gate, up):
        gate_pre = jnp.dot(rows, gate, preferred_element_type=F32)
        return gate_pre * jax.nn.sigmoid(gate_pre) * jnp.dot(rows, up, preferred_element_type=F32)

    rows = moe[...]
    lane = lax.broadcasted_iota(jnp.int32, (n * seq, route.shape[-1]), 1)
    weights = route[...].reshape(n * seq, route.shape[-1])
    hidden = []
    for e in range(exp_local):
        weight = jnp.sum(
            jnp.where(lane == me * exp_local + e, weights, 0.0), axis=1, keepdims=True
        )
        hidden.append((swiglu(rows, egate[e], eup[e]) * weight).astype(BF16))
    dense = swiglu(rows, dgate[...], dup[...]).astype(BF16)
    shared = swiglu(moe[span(me, seq), :], sgate[...], sup[...]).astype(BF16)
    for copy in wcopies:
        copy.wait()

    def compute(t):
        at = span(t, cols)
        value = mix[t, 0:1, :] * jnp.dot(dense, ddown[:, at], preferred_element_type=F32)
        for e in range(exp_local):
            value = value + jnp.dot(hidden[e], edown[e, :, at], preferred_element_type=F32)
        part[t] = value.astype(BF16)
        spart[t] = jnp.dot(shared, sdown[:, at], preferred_element_type=F32).astype(BF16)

    order = [2 * s + 1 for s in list(range(1, half)) + [0]]
    order += [2 * s for s in range(1, half)] + [n, 0]
    turns = list(range(1, sides)) + [0]

    def piece(s, t):
        if s == n:
            return spart.at[t]
        return part.at[t, span(to(s // 2, s % 2), seq), :]

    c2, y2, e2, x2 = {}, {}, {}, {}
    last = None
    for q in turns:
        other = lax.rem(side + q, sides) * CORES + (CORES - 1 - core)
        compute(other)
        for s in order:
            i = s * sides + q
            copy = send(piece(s, other), crecv.at[i], c2sems, i, {"tp": twin})
            copy.start()
            c2[s, q] = copy
        peer = lax.rem(side + q, sides) * CORES + core
        compute(peer)
        for s in order:
            i = s * sides + q
            c2[s, q].wait_recv()
            both = piece(s, peer)[...].astype(F32) + crecv[i].astype(F32)
            if q:
                ysend[i] = both.astype(BF16)
                copy = send(ysend.at[i], yrecv.at[i], y2sems, i, {"tp": peer})
                copy.start()
                y2[s, q] = copy
                continue
            for z in turns[:-1]:
                y2[s, z].wait_recv()
                both = both + yrecv[i + z].astype(F32)
            far = s // 2
            if s < n and s % 2 == 0:
                x2[far].wait_recv()
                both = both + xrecv[far].astype(F32)
            if s < n and s % 2:
                esend[s] = both.astype(BF16)
                copy = send(esend.at[s], xrecv.at[far], x2sems, far, {"ep": mate})
                copy.start()
                x2[far] = copy
            elif 0 < s < n:
                esend[s] = both.astype(BF16)
                copy = send(esend.at[s], erecv.at[far], e2sems, far, {"ep": to(far, 0)})
                copy.start()
                e2[far] = copy
            else:
                last = both if last is None else last + both
    last = last + resid[...]
    for s in range(1, half):
        e2[s].wait_recv()
        last = last + erecv[s].astype(F32)
    out[...] = last.astype(BF16)
    for copy in hcopies + qcopies:
        copy.wait_send()
    for group in (ycopies, ecopies, xcopies, c2, y2, e2, x2):
        for copy in group.values():
            copy.wait_send()


def pairs(counts):
    return [pltpu.SemaphoreType.DMA((c,)) for c in counts for _ in range(2)]


def call(kernel, outs, ins, spaces, out_spaces, scratch, ident):
    return pl.pallas_call(
        kernel,
        out_shape=outs,
        in_specs=[pl.BlockSpec(memory_space=s) for s in spaces],
        out_specs=[pl.BlockSpec(memory_space=s) for s in out_spaces],
        scratch_shapes=scratch,
        compiler_params=pltpu.CompilerParams(
            collective_id=ident, has_side_effects=True, vmem_limit_bytes=VMEM_BYTES
        ),
    )(*ins)


def local(
    tokens,
    state,
    norm_gain,
    w_query,
    w_forget,
    w_input,
    w_outgate,
    lower_bound,
    head_gain,
    w_output,
    ffn_gain,
    route_ids,
    route_weight,
    expert_gate,
    expert_up,
    expert_down,
    shared_gate,
    shared_up,
    shared_down,
    dense_gate,
    dense_up,
    dense_down,
    dense_mix,
):
    n = lax.axis_size("ep")
    tpn = lax.axis_size("tp")
    seq, width = tokens.shape
    depth, mix_local = w_query.shape
    heads_local = state.shape[1]
    head_dim = state.shape[2]
    cols = width // tpn
    exp_local = expert_gate.shape[0]
    experts = exp_local * n
    slots = -(-experts // LANES) * LANES
    sds = jax.ShapeDtypeStruct
    VM, ANY = pltpu.VMEM, pl.ANY

    dense_cols = dense_gate.shape[1] // tpn
    move = dense_cols % LANES == 0
    ins = [tokens, norm_gain[None, :], route_ids, route_weight, dense_mix[None, :]]
    ins += [w_query, w_forget, w_input, w_outgate]
    outs = [
        sds((seq, 4 * mix_local), BF16),
        sds((n, seq, slots), F32),
        sds((tpn, 8, cols), F32),
    ]
    half = n // 2
    scratch = [
        VM((seq, slots), F32),
        VM((8, cols), F32),
        VM((n, seq, depth), BF16),
        VM((n, seq, depth), BF16),
        VM((n, seq, 4 * mix_local), BF16),
        VM((half, seq, 4 * mix_local), BF16),
        VM((half, seq, 4 * mix_local), BF16),
    ] + pairs([n, n, half, tpn, half])
    spaces, out_spaces = [VM] * len(ins), [VM] * len(outs)
    if move:
        ins += [dense_gate, dense_up]
        outs += [sds((width, dense_cols), BF16)] * 2
        spaces += [ANY] * 2
        out_spaces += [ANY] * 2
        scratch += pairs([2 * tpn]) + [pltpu.SemaphoreType.DMA((2,))]
    res = call(
        functools.partial(front_kernel, n, tpn, move), outs, ins, spaces, out_spaces, scratch, 0
    )
    projected, route_all, mix_all = res[:3]
    if move:
        gate_w, up_w = res[3:]
        down_w = dense_down
    else:
        gate_w, up_w = [
            lax.all_to_all(w, "tp", split_axis=1, concat_axis=0, tiled=True)
            for w in (dense_gate, dense_up)
        ]
        down_w = lax.all_to_all(dense_down, "tp", split_axis=0, concat_axis=1, tiled=True)

    step = 8
    new_state, head_out = pl.pallas_call(
        state_kernel,
        grid=(seq // step,),
        out_shape=[sds(state.shape, F32), sds((seq, mix_local), BF16)],
        in_specs=[
            pl.BlockSpec((step, 4 * mix_local), lambda i: (i, 0)),
            pl.BlockSpec((1, mix_local), lambda i: (0, 0)),
            pl.BlockSpec((1, mix_local), lambda i: (0, 0)),
            pl.BlockSpec((step,) + state.shape[1:], lambda i: (i, 0, 0, 0)),
        ],
        out_specs=[
            pl.BlockSpec((step,) + state.shape[1:], lambda i: (i, 0, 0, 0)),
            pl.BlockSpec((step, mix_local), lambda i: (i, 0)),
        ],
    )(projected, lower_bound[None, :], head_gain[None, :], state)

    sides = tpn // CORES
    blocks = (n + 1) * sides
    big = [expert_gate, expert_up, expert_down, shared_gate, shared_up, shared_down]
    big += [gate_w, up_w, down_w]
    held = [VM(w.shape, BF16) for w in big]
    if move:
        held[8] = VM((dense_cols, width), BF16)
    (mixed,) = call(
        functools.partial(main_kernel, n, tpn, move),
        [sds((seq, cols), BF16)],
        [tokens, ffn_gain[None, :], head_out, w_output, route_all, mix_all] + big,
        [VM] * 6 + [ANY] * 9,
        [VM],
        [
            VM((n * seq, width), BF16),
            VM((seq, cols), F32),
            VM((tpn, seq, cols), BF16),
            VM((tpn, seq, cols), BF16),
            VM((seq, LANES), F32),
            VM((tpn, seq, LANES), F32),
        ]
        + held
        + [VM((tpn, n * seq, cols), BF16), VM((tpn, seq, cols), BF16)]
        + [VM((blocks, seq, cols), BF16)] * 3
        + [VM((n, seq, cols), BF16)]
        + [VM((half, seq, cols), BF16)] * 2
        + pairs([tpn, tpn, half, n * sides, n * sides, blocks, blocks, half, tpn, half, half])
        + [pltpu.SemaphoreType.DMA((9,))],
        1,
    )
    return (mixed, new_state)


def solution(mesh):
    placed = (
        P("ep", None),
        P("ep", "tp", None, None),
        P(),
        P("ep", "tp"),
        P("ep", "tp"),
        P("ep", "tp"),
        P("ep", "tp"),
        P("tp"),
        P("tp"),
        P("tp", None),
        P(),
        P("ep", None),
        P("ep", None),
        P("ep", None, "tp"),
        P("ep", None, "tp"),
        P("ep", "tp", None),
        P(None, "tp"),
        P(None, "tp"),
        P("tp", None),
        P("tp", "ep"),
        P("tp", "ep"),
        P("ep", "tp"),
        P("tp"),
    )
    return jax.shard_map(
        local,
        mesh=mesh,
        in_specs=placed,
        out_specs=(P("ep", "tp"), P("ep", "tp", None, None)),
        check_vma=False,
    )
```
